32 devices in a mesh: rep: 2 (over x), fs: 8 (over z, y), tp: 2 (over core).
Axes of the slice: x: 2, y: 2, z: 4, core: 2. Of those that a mesh axis runs over, the one named last changes fastest.
Arguments:
- tokens_in: bfloat16 [4096, 2048], P(('rep', 'fs', 'tp')), may hold values from -6 to 6
- norm_gains: float32 [3, 2048], replicated, may hold values from 0.1 to 1.9
- gate_w: float32 [2048, 3072], P('fs', 'tp'), may hold values from -0.125 to 0.125
- gate_scale: float32 [3072], P('tp'), may hold values from 0.5 to 2
- up_w: float32 [2048, 3072], P('fs', 'tp'), may hold values from -0.125 to 0.125
- up_scale: float32 [3072], P('tp'), may hold values from 0.5 to 2
- down_w: float32 [3072, 2048], P('tp', 'fs'), may hold values from -0.109375 to 0.109375
- down_scale: float32 [2048], P('fs'), may hold values from 0.5 to 2
- query_w: float32 [2048, 2048], P('fs', 'tp'), may hold values from -0.125 to 0.125
- query_scale: float32 [2048], P('tp'), may hold values from 0.5 to 2
- key_w: float32 [2048, 2048], P('fs', 'tp'), may hold values from -0.125 to 0.125
- key_scale: float32 [2048], P('tp'), may hold values from 0.5 to 2
- value_w: float32 [2048, 2048], P('fs', 'tp'), may hold values from -0.125 to 0.125
- value_scale: float32 [2048], P('tp'), may hold values from 0.5 to 2
- out_w: float32 [2048, 2048], P('tp', 'fs'), may hold values from -0.125 to 0.125
- out_scale: float32 [2048], P('fs'), may hold values from 0.5 to 2
- head_gain: float32 [256], replicated, may hold values from 0.1 to 1.9
- decay_rate: float32 [8], P('tp'), may hold values from 0 to 1, as said below
Outputs:
- tokens_out: bfloat16 [4096, 2048], P(('rep', 'fs', 'tp'))
The draws below stay inside these ranges and needn't reach their ends.
Inputs may be any that keep to these rules, and one draw needn't show every extreme that they name: `decay_rate`: each head's decay per position, positive.
All inputs are finite; a program needn't handle non-finite values.
Results may differ from the reference program's by a relative error of at most 0.02.
Values may be sent and summed in bfloat16 or wider, within the bound.
A program may use at most 128 MiB of HBM per device.

```python
import math
import jax
import jax.numpy as jnp
from jax import lax

D = 2048
FF = 3072
HEADS = 8
DK = 256
DV = 256
BLOCK = 64
SEQ = 256
TOKENS = 4096
N_TP = 2


def draw_decay_rate(key, part):
    uniform_draw = jax.random.uniform(key, (HEADS,), jnp.float32)
    lowest, highest = (0.5, 16.0)
    spread = jnp.log(highest) - jnp.log(lowest)
    return jnp.exp(jnp.log(lowest) + uniform_draw * spread) / SEQ


def steps_of(rng, shape, shards, least, high):
    level, own = 1.0, jax.random.fold_in(rng, 6)
    for dim, shards_of in shards:
        heights = jnp.exp(jax.random.uniform(jax.random.fold_in(own, dim), (shards_of,), jnp.float32, least / len(shards), high / len(shards)))
        level = level * jnp.repeat(heights, shape[dim] // shards_of).reshape([-1 if axis == dim else 1 for axis in range(len(shape))])
    return level


def noise(own_key, shape, width, most, cuts=(), held_as=jnp.bfloat16):
    drawn = jax.random.normal(own_key, shape, jnp.float32) * width
    if len(cuts) > 0:
        drawn = steps_of(own_key, shape, cuts, -0.22, 0.18) * drawn
    return jnp.clip(drawn, min=-most, max=most).astype(held_as)


def setup_inputs(seed: int = 0) -> dict:
    streams_of = jax.random.split(jax.random.key(seed), 19)
    tokens_in = noise(streams_of[0], (TOKENS, D), 1.0, 6.0, ((0, 32),))
    norm_gains = jnp.clip(1.0 + 0.18 * jax.random.normal(streams_of[1], (3, D), jnp.float32), 0.1, 1.9)
    gate_w = noise(streams_of[2], (D, FF), D ** -0.5, 0.125, ((0, 8), (1, 2)), jnp.float32)
    gate_scale = jnp.clip(jnp.exp(math.log(2.0) - 1.3862944 * jax.random.uniform(streams_of[3], (FF,), jnp.float32) ** steps_of(streams_of[3], (FF,), ((0, 2),), -0.2, 0.2)), 0.5, 2.0)
    up_w = noise(streams_of[4], (D, FF), D ** -0.5, 0.125, ((0, 8), (1, 2)), jnp.float32)
    up_scale = jnp.clip(jnp.exp(math.log(2.0) - 1.3862944 * jax.random.uniform(streams_of[5], (FF,), jnp.float32) ** steps_of(streams_of[5], (FF,), ((0, 2),), -0.2, 0.2)), 0.5, 2.0)
    down_w = noise(streams_of[6], (FF, D), FF ** -0.5, 0.109375, ((0, 2), (1, 8)), jnp.float32)
    down_scale = jnp.clip(jnp.exp(math.log(2.0) - 1.3862944 * jax.random.uniform(streams_of[7], (D,), jnp.float32) ** steps_of(streams_of[7], (D,), ((0, 8),), -0.2, 0.2)), 0.5, 2.0)
    query_w = noise(streams_of[8], (D, HEADS * DK), D ** -0.5, 0.125, ((0, 8), (1, 2)), jnp.float32)
    query_scale = jnp.clip(jnp.exp(math.log(2.0) - 1.3862944 * jax.random.uniform(streams_of[9], (HEADS * DK,), jnp.float32) ** steps_of(streams_of[9], (HEADS * DK,), ((0, 2),), -0.2, 0.2)), 0.5, 2.0)
    key_w = noise(streams_of[10], (D, HEADS * DK), D ** -0.5, 0.125, ((0, 8), (1, 2)), jnp.float32)
    key_scale = jnp.clip(jnp.exp(math.log(2.0) - 1.3862944 * jax.random.uniform(streams_of[11], (HEADS * DK,), jnp.float32) ** steps_of(streams_of[11], (HEADS * DK,), ((0, 2),), -0.2, 0.2)), 0.5, 2.0)
    value_w = noise(streams_of[12], (D, HEADS * DV), D ** -0.5, 0.125, ((0, 8), (1, 2)), jnp.float32)
    value_scale = jnp.clip(jnp.exp(math.log(2.0) - 1.3862944 * jax.random.uniform(streams_of[13], (HEADS * DV,), jnp.float32) ** steps_of(streams_of[13], (HEADS * DV,), ((0, 2),), -0.2, 0.2)), 0.5, 2.0)
    out_w = noise(streams_of[14], (HEADS * DV, D), (HEADS * DV) ** -0.5, 0.125, ((0, 2), (1, 8)), jnp.float32)
    out_scale = jnp.clip(jnp.exp(math.log(2.0) - 1.3862944 * jax.random.uniform(streams_of[15], (D,), jnp.float32) ** steps_of(streams_of[15], (D,), ((0, 8),), -0.2, 0.2)), 0.5, 2.0)
    head_gain = jnp.clip(1.0 + 0.18 * jax.random.normal(streams_of[16], (DV,), jnp.float32), 0.1, 1.9)
    decay_rate = draw_decay_rate(jax.random.fold_in(streams_of[18], 71), 0)
    return dict(tokens_in=tokens_in, norm_gains=norm_gains, gate_w=gate_w, gate_scale=gate_scale, up_w=up_w, up_scale=up_scale, down_w=down_w, down_scale=down_scale, query_w=query_w, query_scale=query_scale, key_w=key_w, key_scale=key_scale, value_w=value_w, value_scale=value_scale, out_w=out_w, out_scale=out_scale, head_gain=head_gain, decay_rate=decay_rate)


EPSILON = 1e-05

def rms_scale(stream, gain):
    return stream * lax.rsqrt(lax.optimization_barrier(jnp.mean(stream * stream, axis=-1, keepdims=True)) + EPSILON) * gain

def group_sum(hidden, weight, scale):
    groups = hidden.reshape(hidden.shape[0], N_TP, -1).transpose(1, 0, 2)
    blocks_w = weight.reshape(N_TP, -1, weight.shape[1])

    def one_group(operands):
        rounded = (jnp.dot(operands[0], operands[1], preferred_element_type=jnp.float32) * scale).astype(jnp.bfloat16)
        return lax.optimization_barrier(rounded).astype(jnp.float32)
    return lax.optimization_barrier(jnp.sum(lax.map(one_group, (groups, blocks_w)), axis=0))

def feed_forward(stream, gain, weights, scales):
    gate_b, up_b, down_b = weights
    normed = rms_scale(stream, gain).astype(jnp.bfloat16)
    gate_value = jnp.dot(normed, gate_b, preferred_element_type=jnp.float32) * scales[0]
    up_value = jnp.dot(normed, up_b, preferred_element_type=jnp.float32) * scales[1]
    hidden = (jax.nn.silu(gate_value) * up_value).astype(jnp.bfloat16)
    return group_sum(hidden, down_b, scales[2])

def retention(query, key_rows, value, decay_rate, head_gain):
    seq_len = query.shape[0]
    blocks = seq_len // BLOCK
    q_heads = query.astype(jnp.float32).reshape(blocks, BLOCK, HEADS, DK).transpose(0, 2, 1, 3)
    k_heads = key_rows.astype(jnp.float32).reshape(blocks, BLOCK, HEADS, DK).transpose(0, 2, 1, 3)
    v_heads = value.astype(jnp.float32).reshape(blocks, BLOCK, HEADS, DV).transpose(0, 2, 1, 3)
    offsets = jnp.arange(BLOCK, dtype=jnp.float32)
    inner_decay = jnp.exp(-decay_rate[:, None, None] * jnp.abs(offsets[:, None] - offsets[None, :]))
    query_decay = jnp.exp(-decay_rate[:, None] * offsets[None, :])[..., None]
    key_decay = jnp.exp(-decay_rate[:, None] * (BLOCK - offsets)[None, :])[..., None]
    block_decay = jnp.exp(-decay_rate * BLOCK)[:, None, None]

    def advance(state, inputs):
        q_blk, k_blk, v_blk = inputs
        scores = (jnp.einsum('hid,hjd->hij', q_blk, k_blk) * inner_decay).astype(jnp.bfloat16)
        scores = lax.optimization_barrier(scores).astype(jnp.float32)
        within = jnp.einsum('hij,hje->hie', scores, v_blk)
        carried = jnp.einsum('hid,hde->hie', q_blk * query_decay, state, precision=lax.Precision.HIGHEST)
        state = state * block_decay + jnp.einsum('hjd,hje->hde', k_blk * key_decay, v_blk, precision=lax.Precision.HIGHEST)
        return (state, within + carried)
    initial = jnp.zeros((HEADS, DK, DV), jnp.float32)
    _, retained = lax.scan(advance, initial, (q_heads, k_heads, v_heads))
    retained = retained.transpose(0, 2, 1, 3).reshape(seq_len, HEADS, DV)
    centred = retained - lax.optimization_barrier(jnp.mean(retained, axis=-1, keepdims=True))
    normed = centred * lax.rsqrt(lax.optimization_barrier(jnp.mean(centred * centred, axis=-1, keepdims=True)) + EPSILON) * head_gain
    return normed.reshape(seq_len, HEADS * DV).astype(jnp.bfloat16)

def reference(tokens_in, norm_gains, gate_w, gate_scale, up_w, up_scale, down_w, down_scale, query_w, query_scale, key_w, key_scale, value_w, value_scale, out_w, out_scale, head_gain, decay_rate):
    ffn_weights = (gate_w.astype(jnp.bfloat16), up_w.astype(jnp.bfloat16), down_w.astype(jnp.bfloat16))
    ffn_scales = (gate_scale, up_scale, down_scale)
    query_b = query_w.astype(jnp.bfloat16)
    key_b = key_w.astype(jnp.bfloat16)
    value_b = value_w.astype(jnp.bfloat16)
    out_b = out_w.astype(jnp.bfloat16)

    def one_sequence(stream_in):
        stream = stream_in.astype(jnp.float32)
        first = stream + 0.5 * feed_forward(stream, norm_gains[0], ffn_weights, ffn_scales)
        normed = rms_scale(first, norm_gains[1]).astype(jnp.bfloat16)
        query = (jnp.dot(normed, query_b, preferred_element_type=jnp.float32) * query_scale).astype(jnp.bfloat16)
        key_rows = (jnp.dot(normed, key_b, preferred_element_type=jnp.float32) * key_scale / math.sqrt(DK)).astype(jnp.bfloat16)
        value = (jnp.dot(normed, value_b, preferred_element_type=jnp.float32) * value_scale).astype(jnp.bfloat16)
        mixed = retention(query, key_rows, value, decay_rate, head_gain)
        second = first + group_sum(mixed, out_b, out_scale)
        final = second + 0.5 * feed_forward(second, norm_gains[2], ffn_weights, ffn_scales)
        return final.astype(jnp.bfloat16)
    sequences = tokens_in.reshape(-1, SEQ, D)
    return lax.map(one_sequence, sequences).reshape(-1, D)
```

```python
import math

import jax
import jax.numpy as jnp
from jax import lax
from jax.sharding import PartitionSpec as P

DK = 256
DV = 256
BLOCK = 64

EPSILON = 1e-05


def rms_scale(stream, gain):
    return stream * lax.rsqrt(jnp.mean(stream * stream, axis=-1, keepdims=True) + EPSILON) * gain


def snake(n):
    return [i for i in range(0, n, 2)] + [i for i in range(n - 1, 0, -1) if i % 2 == 1]


def snake_place(index, n):
    return jnp.where(index % 2 == 0, index // 2, n - 1 - index // 2)


def snake_index(place, n):
    half = (n + 1) // 2
    return jnp.where(place < half, 2 * place, 2 * (n - 1 - place) + 1)


def shift(x, axis, n, by):
    return lax.ppermute(x, axis, [(i, (i + by) % n) for i in range(n)])


def ring_gather(shards, n, forward_steps):
    order = snake(n)
    ahead = [(order[i], order[(i + 1) % n]) for i in range(n)]
    behind = [(b, a) for a, b in ahead]
    found = []
    for x, steps in zip(shards, forward_steps):
        forward, back = [x], [x]
        found.append((forward, back))
    for step in range(n):
        for (forward, back), steps in zip(found, forward_steps):
            if step < steps:
                forward.append(lax.ppermute(forward[-1], "fs", ahead))
            if step < n - 1 - steps:
                back.append(lax.ppermute(back[-1], "fs", behind))
    return [forward + back[:0:-1] for forward, back in found]


def chained(shards, before):
    if not before:
        return shards
    last = []
    n = len(before[0])
    for pieces in before:
        last.extend([pieces[n // 2], pieces[(n // 2 + 1) % n]])
    return lax.optimization_barrier((tuple(shards), tuple(last)))[0]


def retain(query, key_rows, value, decay, head_gain):
    seq_len = query.shape[0]
    row = lax.broadcasted_iota(jnp.int32, (seq_len, seq_len), 0)
    col = lax.broadcasted_iota(jnp.int32, (seq_len, seq_len), 1)
    distance = jnp.abs(row - col).astype(jnp.float32)
    weight = jnp.where(col // BLOCK <= row // BLOCK, jnp.exp(-decay * distance), 0.0)
    scores = lax.dot_general(
        query, key_rows, (((1,), (1,)), ((), ())), preferred_element_type=jnp.float32
    )
    scores = (scores * weight).astype(jnp.bfloat16)
    retained = jnp.dot(scores, value, preferred_element_type=jnp.float32)
    centred = retained - jnp.mean(retained, axis=-1, keepdims=True)
    normed = (
        centred
        * lax.rsqrt(jnp.mean(centred * centred, axis=-1, keepdims=True) + EPSILON)
        * head_gain
    )
    return normed.astype(jnp.bfloat16)


def on_device(
    n_rep,
    n_fs,
    n_tp,
    tokens_in,
    norm_gains,
    gate_w,
    gate_scale,
    up_w,
    up_scale,
    down_w,
    down_scale,
    query_w,
    query_scale,
    key_w,
    key_scale,
    value_w,
    value_scale,
    out_w,
    out_scale,
    head_gain,
    decay_rate,
):
    rows = tokens_in.shape[0]
    width = gate_w.shape[0]
    heads = decay_rate.shape[0]
    units = gate_w.shape[1]
    share = n_rep if heads % n_rep == 0 and units % (n_rep * 128) == 0 else 1
    heads //= share
    units //= share
    rep = lax.axis_index("rep") if share > 1 else 0
    tp = lax.axis_index("tp")
    place = snake_place(lax.axis_index("fs"), n_fs)

    def part(x, axis):
        size = x.shape[axis] // share
        return lax.dynamic_slice_in_dim(x, rep * size, size, axis)

    def halves(x):
        size = x.shape[0] // 2
        return [x[:size], x[size:]]

    gate_b, up_b, query_b, key_b, value_b = (
        part(w, 1).astype(jnp.bfloat16) for w in (gate_w, up_w, query_w, key_w, value_w)
    )
    down_b, out_b = (part(w, 0).astype(jnp.bfloat16) for w in (down_w, out_w))

    few, many = (n_fs - 1) // 2, n_fs // 2
    (scales,) = ring_gather([jnp.stack([down_scale, out_scale])], n_fs, [few])
    first_pieces = ring_gather([gate_b, up_b], n_fs, [few, many])
    down_pieces = ring_gather(chained(halves(down_b), first_pieces), n_fs, [few, many])
    query_pieces = ring_gather(chained([query_b, key_b], down_pieces), n_fs, [few, many])
    value_pieces = ring_gather(
        chained([value_b] + halves(out_b), query_pieces), n_fs, [few, many, many]
    )

    gate_full, up_full = (jnp.concatenate(p, axis=0) for p in first_pieces)
    down_full = jnp.concatenate([jnp.concatenate(p, axis=1) for p in down_pieces], axis=0)
    query_full, key_full = (jnp.concatenate(p, axis=0) for p in query_pieces)
    value_full = jnp.concatenate(value_pieces[0], axis=0)
    out_full = jnp.concatenate([jnp.concatenate(p, axis=1) for p in value_pieces[1:]], axis=0)
    down_cols, out_cols = jnp.split(jnp.concatenate(scales, axis=1), 2, axis=0)

    def to_ring(x):
        blocks = [
            lax.dynamic_slice_in_dim(
                x, snake_index((place - k) % n_fs, n_fs) * width, width, axis=1
            )
            for k in range(n_fs)
        ]
        return jnp.concatenate(blocks, axis=1)

    def from_ring(x):
        blocks = [
            lax.dynamic_slice_in_dim(x, (place - snake(n_fs).index(o)) % n_fs * width, width, axis=1)
            for o in range(n_fs)
        ]
        return jnp.concatenate(blocks, axis=1)

    def over_tp(x):
        found = [x] + [shift(x, "tp", n_tp, k) for k in range(1, n_tp)]
        twice = jnp.concatenate(found[::-1] * 2, axis=0)
        return lax.dynamic_slice_in_dim(twice, (n_tp - 1 - tp) * rows, n_tp * rows, axis=0)

    def gather_rows(normed):
        found = [normed] + [shift(normed, "rep", n_rep, k) for k in range(1, share)]
        return [over_tp(x) for x in found]

    def return_rows(parts):
        total = None
        for k in range(share - 1, -1, -1):
            mine = lax.dynamic_slice_in_dim(parts[k], tp * rows, rows, axis=0)
            for j in range(1, n_tp):
                other = lax.dynamic_slice_in_dim(parts[k], (tp + j) % n_tp * rows, rows, axis=0)
                mine = mine + shift(other.astype(jnp.bfloat16), "tp", n_tp, j).astype(jnp.float32)
            if k > 0:
                mine = shift(mine.astype(jnp.bfloat16), "rep", n_rep, n_rep - k).astype(jnp.float32)
            total = mine if total is None else total + mine
        return total

    def dot(a, b):
        return jnp.dot(a, b, preferred_element_type=jnp.float32)

    gate_col, up_col = part(gate_scale, 0), part(up_scale, 0)

    def feed_forward(stream, gain):
        parts = []
        for gathered in gather_rows(rms_scale(stream, gain).astype(jnp.bfloat16)):
            gate_value = dot(gathered, gate_full) * gate_col
            up_value = dot(gathered, up_full) * up_col
            hidden = (jax.nn.silu(gate_value) * up_value).astype(jnp.bfloat16)
            parts.append(dot(hidden, down_full) * down_cols)
        return return_rows(parts)

    query_col, key_col, value_col = (part(s, 0) for s in (query_scale, key_scale, value_scale))
    decay = part(decay_rate, 0)
    gains = to_ring(norm_gains)

    stream = to_ring(tokens_in).astype(jnp.float32)
    stream = stream + 0.5 * feed_forward(stream, gains[0])
    parts = []
    for gathered in gather_rows(rms_scale(stream, gains[1]).astype(jnp.bfloat16)):
        query = (dot(gathered, query_full) * query_col).astype(jnp.bfloat16)
        key_rows = (dot(gathered, key_full) * key_col / math.sqrt(DK)).astype(jnp.bfloat16)
        value = (dot(gathered, value_full) * value_col).astype(jnp.bfloat16)
        mixed = [
            retain(
                query[:, h * DK : (h + 1) * DK],
                key_rows[:, h * DK : (h + 1) * DK],
                value[:, h * DV : (h + 1) * DV],
                decay[h],
                head_gain,
            )
            for h in range(heads)
        ]
        parts.append(dot(jnp.concatenate(mixed, axis=1), out_full) * out_cols)
    stream = stream + return_rows(parts)
    stream = stream + 0.5 * feed_forward(stream, gains[2])
    return from_ring(stream.astype(jnp.bfloat16))


def solution(mesh):
    sizes = [mesh.shape[axis] for axis in ("rep", "fs", "tp")]
    placed = (
        P(("rep", "fs", "tp"), None),
        P(),
        P("fs", "tp"),
        P("tp"),
        P("fs", "tp"),
        P("tp"),
        P("tp", "fs"),
        P("fs"),
        P("fs", "tp"),
        P("tp"),
        P("fs", "tp"),
        P("tp"),
        P("fs", "tp"),
        P("tp"),
        P("tp", "fs"),
        P("fs"),
        P(),
        P("tp"),
    )
    return jax.shard_map(
        lambda *args: on_device(*sizes, *args),
        mesh=mesh,
        in_specs=placed,
        out_specs=P(("rep", "fs", "tp"), None),
        check_vma=False,
    )
```

```python
import math

import jax
import jax.numpy as jnp
from jax import lax
from jax.sharding import PartitionSpec as P

DK = 256
DV = 256
BLOCK = 64

EPSILON = 1e-05


def rms_scale(stream, gain):
    return stream * lax.rsqrt(jnp.mean(stream * stream, axis=-1, keepdims=True) + EPSILON) * gain


def snake(n):
    return [i for i in range(0, n, 2)] + [i for i in range(n - 1, 0, -1) if i % 2 == 1]


def snake_place(index, n):
    return jnp.where(index % 2 == 0, index // 2, n - 1 - index // 2)


def snake_index(place, n):
    half = (n + 1) // 2
    return jnp.where(place < half, 2 * place, 2 * (n - 1 - place) + 1)


def shift(x, axis, n, by):
    return lax.ppermute(x, axis, [(i, (i + by) % n) for i in range(n)])


def ring_gather(shards, n, forward_steps):
    order = snake(n)
    ahead = [(order[i], order[(i + 1) % n]) for i in range(n)]
    behind = [(b, a) for a, b in ahead]
    found = []
    for x, steps in zip(shards, forward_steps):
        forward, back = [x], [x]
        found.append((forward, back))
    for step in range(n):
        for (forward, back), steps in zip(found, forward_steps):
            if step < steps:
                forward.append(lax.ppermute(forward[-1], "fs", ahead))
            if step < n - 1 - steps:
                back.append(lax.ppermute(back[-1], "fs", behind))
    return [forward + back[:0:-1] for forward, back in found]


def chained(shards, before, hops):
    if not before:
        return shards
    last = []
    n = len(before[0])
    for pieces in before:
        last.extend([pieces[hops], pieces[n - hops]])
    return lax.optimization_barrier((tuple(shards), tuple(last)))[0]


def with_scale(weight, scale):
    high = lax.reduce_precision(scale, 8, 7)
    middle = lax.reduce_precision(scale - high, 8, 7)
    rows = jnp.stack([high, middle, scale - high - middle]).astype(jnp.bfloat16)
    return jnp.concatenate([weight, jnp.pad(rows, ((0, 13), (0, 0)))], axis=0)


def without_scale(pieces):
    size = pieces[0].shape[0] - 16
    weight = jnp.concatenate([p[:size] for p in pieces], axis=1)
    rows = jnp.concatenate([p[size:] for p in pieces], axis=1)[:3].astype(jnp.float32)
    return weight, rows[0] + rows[1] + rows[2]


def retain(query, key_rows, value, decay, head_gain):
    seq_len = query.shape[0]
    row = lax.broadcasted_iota(jnp.int32, (seq_len, seq_len), 0)
    col = lax.broadcasted_iota(jnp.int32, (seq_len, seq_len), 1)
    distance = jnp.abs(row - col).astype(jnp.float32)
    weight = jnp.where(col // BLOCK <= row // BLOCK, jnp.exp(-decay * distance), 0.0)
    scores = lax.dot_general(
        query, key_rows, (((1,), (1,)), ((), ())), preferred_element_type=jnp.float32
    )
    scores = (scores * weight).astype(jnp.bfloat16)
    retained = jnp.dot(scores, value, preferred_element_type=jnp.float32)
    centred = retained - jnp.mean(retained, axis=-1, keepdims=True)
    normed = (
        centred
        * lax.rsqrt(jnp.mean(centred * centred, axis=-1, keepdims=True) + EPSILON)
        * head_gain
    )
    return normed.astype(jnp.bfloat16)


def on_device(
    n_rep,
    n_fs,
    n_tp,
    tokens_in,
    norm_gains,
    gate_w,
    gate_scale,
    up_w,
    up_scale,
    down_w,
    down_scale,
    query_w,
    query_scale,
    key_w,
    key_scale,
    value_w,
    value_scale,
    out_w,
    out_scale,
    head_gain,
    decay_rate,
):
    rows = tokens_in.shape[0]
    width = gate_w.shape[0]
    heads = decay_rate.shape[0]
    units = gate_w.shape[1]
    share = n_rep if heads % n_rep == 0 and units % (n_rep * 128) == 0 else 1
    heads //= share
    units //= share
    rep = lax.axis_index("rep") if share > 1 else 0
    tp = lax.axis_index("tp")
    place = snake_place(lax.axis_index("fs"), n_fs)

    def part(x, axis):
        size = x.shape[axis] // share
        return lax.dynamic_slice_in_dim(x, rep * size, size, axis)

    gate_b, up_b, query_b, key_b, value_b = (
        part(w, 1).astype(jnp.bfloat16) for w in (gate_w, up_w, query_w, key_w, value_w)
    )
    down_b, out_b = (part(w, 0).astype(jnp.bfloat16) for w in (down_w, out_w))

    few, many = (n_fs - 1) // 2, n_fs // 2
    first_pieces = ring_gather([gate_b, up_b], n_fs, [many, few])
    half = down_b.shape[0] // 2
    second_pieces = ring_gather(
        chained([with_scale(down_b[:half], down_scale), down_b[half:]], first_pieces, max(1, n_fs // 4)),
        n_fs,
        [many, few],
    )
    third_pieces = ring_gather(chained([query_b, key_b], second_pieces, few), n_fs, [many, few])
    value_pieces, out_pieces = ring_gather(
        chained([value_b, with_scale(out_b, out_scale)], third_pieces, few), n_fs, [many, few]
    )

    gate_full, up_full = (jnp.concatenate(p, axis=0) for p in first_pieces)
    down_top, down_cols = without_scale(second_pieces[0])
    down_rest = jnp.concatenate(second_pieces[1], axis=1)
    down_full = lax.optimization_barrier(jnp.concatenate([down_top, down_rest], axis=0))
    query_full, key_full = (jnp.concatenate(p, axis=0) for p in third_pieces)
    value_full = jnp.concatenate(value_pieces, axis=0)
    out_full, out_cols = without_scale(out_pieces)

    def to_ring(x):
        blocks = [
            lax.dynamic_slice_in_dim(
                x, snake_index((place - k) % n_fs, n_fs) * width, width, axis=1
            )
            for k in range(n_fs)
        ]
        return jnp.concatenate(blocks, axis=1)

    def from_ring(x):
        blocks = [
            lax.dynamic_slice_in_dim(x, (place - snake(n_fs).index(o)) % n_fs * width, width, axis=1)
            for o in range(n_fs)
        ]
        return jnp.concatenate(blocks, axis=1)

    def over_tp(x, ordered):
        found = [x] + [shift(x, "tp", n_tp, k) for k in range(1, n_tp)]
        if not ordered:
            return jnp.concatenate(found, axis=0)
        twice = jnp.concatenate(found[::-1] * 2, axis=0)
        return lax.dynamic_slice_in_dim(twice, (n_tp - 1 - tp) * rows, n_tp * rows, axis=0)

    def gather_rows(normed, ordered=False):
        found = [normed] + [shift(normed, "rep", n_rep, k) for k in range(1, share)]
        return [over_tp(x, ordered) for x in found]

    def return_rows(parts, ordered=False):
        total = None
        for k in range(share - 1, -1, -1):

            def block(j):
                at = (tp - j) % n_tp * rows if ordered else j * rows
                return lax.dynamic_slice_in_dim(parts[k], at, rows, axis=0)

            mine = block(0)
            for j in range(1, n_tp):
                other = shift(block(j).astype(jnp.bfloat16), "tp", n_tp, n_tp - j)
                mine = mine + other.astype(jnp.float32)
            if k > 0:
                mine = shift(mine.astype(jnp.bfloat16), "rep", n_rep, n_rep - k).astype(jnp.float32)
            total = mine if total is None else total + mine
        return total

    def dot(a, b):
        return jnp.dot(a, b, preferred_element_type=jnp.float32)

    gate_col, up_col = part(gate_scale, 0), part(up_scale, 0)

    def feed_forward(stream, gain):
        parts = []
        for gathered in gather_rows(rms_scale(stream, gain).astype(jnp.bfloat16)):
            gate_value = dot(gathered, gate_full) * gate_col
            up_value = dot(gathered, up_full) * up_col
            hidden = (jax.nn.silu(gate_value) * up_value).astype(jnp.bfloat16)
            hidden = lax.optimization_barrier(hidden)
            parts.append(dot(hidden, down_full) * down_cols)
        return return_rows(parts)

    query_col, key_col, value_col = (part(s, 0) for s in (query_scale, key_scale, value_scale))
    decay = part(decay_rate, 0)
    gains = to_ring(norm_gains)

    stream = to_ring(tokens_in).astype(jnp.float32)
    stream = stream + 0.5 * feed_forward(stream, gains[0])
    parts = []
    for gathered in gather_rows(
        rms_scale(stream, gains[1]).astype(jnp.bfloat16), ordered=True
    ):
        query = (dot(gathered, query_full) * query_col).astype(jnp.bfloat16)
        key_rows = (dot(gathered, key_full) * key_col / math.sqrt(DK)).astype(jnp.bfloat16)
        value = (dot(gathered, value_full) * value_col).astype(jnp.bfloat16)
        mixed = [
            retain(
                query[:, h * DK : (h + 1) * DK],
                key_rows[:, h * DK : (h + 1) * DK],
                value[:, h * DV : (h + 1) * DV],
                decay[h],
                head_gain,
            )
            for h in range(heads)
        ]
        parts.append(dot(jnp.concatenate(mixed, axis=1), out_full) * out_cols)
    stream = stream + return_rows(parts, ordered=True)
    stream = stream + 0.5 * feed_forward(stream, gains[2])
    return from_ring(stream.astype(jnp.bfloat16))


def solution(mesh):
    sizes = [mesh.shape[axis] for axis in ("rep", "fs", "tp")]
    placed = (
        P(("rep", "fs", "tp"), None),
        P(),
        P("fs", "tp"),
        P("tp"),
        P("fs", "tp"),
        P("tp"),
        P("tp", "fs"),
        P("fs"),
        P("fs", "tp"),
        P("tp"),
        P("fs", "tp"),
        P("tp"),
        P("fs", "tp"),
        P("tp"),
        P("tp", "fs"),
        P("fs"),
        P(),
        P("tp"),
    )
    return jax.shard_map(
        lambda *args: on_device(*sizes, *args),
        mesh=mesh,
        in_specs=placed,
        out_specs=P(("rep", "fs", "tp"), None),
        check_vma=False,
    )
```
